32 devices in a mesh: grp: 2 (over x), ep: 16 (over z, y, core).
Axes of the slice: x: 2, y: 2, z: 4, core: 2. Of those that a mesh axis runs over, the one named last changes fastest.
Arguments:
- hidden: bfloat16 [4096, 2048], P(('grp', 'ep')), parts along dimension 0, may hold values from -6 to 6
- state: float32 [2, 4096, 4096], P(None, ('grp', 'ep')), parts along dimension 1, may hold values from -6 to 6
- norm_gain: float32 [2048], replicated, may hold values from 0.1 to 1.9
- w_in: bfloat16 [2048, 1024], P(None, 'ep'), may hold values from -0.125 to 0.125
- lam_re: float32 [64, 64], replicated, may hold values from -1 to -0.1
- lam_im: float32 [64, 64], replicated, may hold values from 0 to 200
- log_step: float32 [64], replicated, may hold values from -4.6 to -0.7
- in_re: float32 [64, 64, 16], replicated, may hold values from -1 to 1
- in_im: float32 [64, 64, 16], replicated, may hold values from -1 to 1
- out_re: float32 [64, 16, 64], replicated, may hold values from -0.75 to 0.75
- out_im: float32 [64, 16, 64], replicated, may hold values from -0.75 to 0.75
- skip: float32 [1024], replicated, may hold values from -4 to 4
- w_glu: bfloat16 [1024, 1024], replicated, may hold values from -0.1875 to 0.1875
- w_out: bfloat16 [1024, 2048], replicated, may hold values from -0.375 to 0.375
- ffn_gain: float32 [2048], replicated, may hold values from 0.1 to 1.9
- w_group: bfloat16 [2048, 4], replicated, may hold values from -0.03125 to 0.03125
- w_route: bfloat16 [2048, 16], replicated, may hold values from -0.03125 to 0.03125
- w_gate: bfloat16 [16, 2048, 512], P('ep'), may hold values from -0.125 to 0.125
- w_up: bfloat16 [16, 2048, 512], P('ep'), may hold values from -0.125 to 0.125
- w_down: bfloat16 [16, 512, 2048], P('ep'), may hold values from -2 to 2
- route_ids: int32 [4096, 2], P(('grp', 'ep')), parts along dimension 0, may hold values from 0 to 15, as said below
Outputs:
- hidden_out: bfloat16 [4096, 2048], P(('grp', 'ep')), parts along dimension 0
- new_state: float32 [2, 4096, 4096], P(None, ('grp', 'ep')), parts along dimension 1
The draws below stay inside these ranges and needn't reach their ends.
There are 2 independent parts, one for each index of `grp`. The reference program is written for one: setup_inputs(seed, part) draws one part's arguments, and reference() takes and returns one part's arrays. A program takes and returns all parts, laid end to end along the dimension named above; an argument that names none is the same for every part. Nothing has to cross between parts.
Inputs may be any that keep to these rules, and one draw needn't show every extreme that they name: `route_ids`: each row names 2 different experts of one expert group (experts g * 4 to g * 4 + 3). Among the rows of one device no expert is named more than 32 times, and in every draw some experts are named exactly 32 times by the rows of every device.
All inputs are finite; a program needn't handle non-finite values.
Results may differ from the reference program's by a relative error of at most 0.013.
Values may be sent and summed in bfloat16 or wider, within the bound.
A program may use at most 128 MiB of HBM per device.

```python
import jax
import jax.numpy as jnp
from jax import lax

D = 2048
S5W = 1024
GROUP_CH = 16
STATE = 64
FFE = 512
EXP_GROUPS = 4
TOPK = 2
SEQ_DEV = 128
SEQS = 2048
EXPERTS = 16
EPG = 4
CAP = 32
GROUPS_S5 = 64
N_EP = 16


def draw_route_ids(key, part):
    base = jax.random.fold_in(key, 11)
    big_key, rest_key = jax.random.split(base)
    big = jax.random.randint(big_key, (), 0, EXP_GROUPS)
    half = SEQ_DEV // 2

    def one_block(block_key):
        order_key, other_key, shift_key, label_key = jax.random.split(block_key, 4)
        order = jax.random.permutation(order_key, SEQ_DEV)
        others = (big + 1 + jax.random.randint(other_key, (SEQ_DEV,), 0, EXP_GROUPS - 1)) % EXP_GROUPS
        by_place = jnp.where(jnp.arange(SEQ_DEV) < half, big, others).astype(jnp.int32)
        group = jnp.zeros((SEQ_DEV,), jnp.int32).at[order].set(by_place)
        member = (group[:, None] == jnp.arange(EXP_GROUPS, dtype=jnp.int32)[None, :]).astype(jnp.int32)
        rank = jnp.sum((jnp.cumsum(member, axis=0) - member) * member, axis=1)
        shift = jax.random.randint(shift_key, (EXP_GROUPS,), 0, EPG)
        labels = jax.vmap(lambda sub: jax.random.permutation(sub, EPG))(jax.random.split(label_key, EXP_GROUPS))
        first = (2 * rank + shift[group]) % EPG
        second = (2 * rank + 1 + shift[group]) % EPG
        one = group * EPG + labels[group, first]
        two = group * EPG + labels[group, second]
        return jnp.stack([one, two], axis=1).astype(jnp.int32)
    blocks = jax.vmap(one_block)(jax.random.split(rest_key, SEQS // SEQ_DEV))
    return blocks.reshape(SEQS, TOPK)


def block_scale(stream_key, extent, cuts, low, top_value):
    def one(axis_at, parts):
        draws = jax.random.uniform(jax.random.fold_in(jax.random.fold_in(stream_key, 6), axis_at), (parts,), jnp.float32, low / len(cuts), top_value / len(cuts))
        return jnp.repeat(jnp.exp(draws), extent[axis_at] // parts).reshape((-1,) + (1,) * (len(extent) - axis_at - 1))

    level = one(*cuts[0])
    for cut in cuts[1:]:
        level = level * one(*cut)
    return level


def gaussian(own_key, extent, scale, most, pieces=(), held_as=jnp.bfloat16):
    array = scale * jax.random.normal(own_key, extent, jnp.float32)
    if pieces:
        array = array * block_scale(own_key, extent, pieces, -0.22, 0.18)
    return jnp.clip(array, -most, most).astype(held_as)


def setup_inputs(seed: int = 0, part: int = 0) -> dict:
    key_list = jax.random.split(jax.random.key(seed), 22)
    own_keys = jax.random.split(jax.random.fold_in(key_list[21], part), 22)
    hidden = gaussian(own_keys[0], (SEQS, D), 1.0, 6.0, ((0, 16),))
    state = gaussian(own_keys[1], (2, SEQS, GROUPS_S5 * STATE), 1.0, 6.0, ((1, 16),), jnp.float32)
    norm_gain = jnp.clip(1.0 + 0.18 * jax.random.normal(key_list[2], (D,), jnp.float32), 0.1, 1.9)
    w_in = gaussian(key_list[3], (D, S5W), D ** -0.5, 0.125, ((1, 16),))
    lam_re = jnp.clip(jax.random.uniform(key_list[4], (GROUPS_S5, STATE), jnp.float32, -1.0, -0.1), -1.0, -0.1)
    lam_im = jnp.clip(jax.random.uniform(key_list[5], (GROUPS_S5, STATE), jnp.float32, 0.0, 200.0), 0.0, 200.0)
    log_step = jnp.clip(jax.random.uniform(key_list[6], (GROUPS_S5,), jnp.float32, -4.6, -0.7), -4.6, -0.7)
    in_re = gaussian(key_list[7], (GROUPS_S5, STATE, GROUP_CH), (2 * GROUP_CH) ** -0.5, 1.0, (), jnp.float32)
    in_im = gaussian(key_list[8], (GROUPS_S5, STATE, GROUP_CH), (2 * GROUP_CH) ** -0.5, 1.0, (), jnp.float32)
    out_re = gaussian(key_list[9], (GROUPS_S5, GROUP_CH, STATE), STATE ** -0.5, 0.75, (), jnp.float32)
    out_im = gaussian(key_list[10], (GROUPS_S5, GROUP_CH, STATE), STATE ** -0.5, 0.75, (), jnp.float32)
    skip = gaussian(key_list[11], (S5W,), 1.0, 4.0, (), jnp.float32)
    w_glu = gaussian(key_list[12], (S5W, S5W), S5W ** -0.5, 0.1875)
    w_out = gaussian(key_list[13], (S5W, D), (S5W // 4) ** -0.5, 0.375)
    ffn_gain = jnp.clip(1.0 + 0.18 * jax.random.normal(key_list[14], (D,), jnp.float32), 0.1, 1.9)
    w_group = gaussian(key_list[15], (D, EXP_GROUPS), (16 * D) ** -0.5, 0.03125)
    w_route = gaussian(key_list[16], (D, EXPERTS), (16 * D) ** -0.5, 0.03125)
    w_gate = gaussian(key_list[17], (EXPERTS, D, FFE), D ** -0.5, 0.125, ((0, 16),))
    w_up = gaussian(key_list[18], (EXPERTS, D, FFE), D ** -0.5, 0.125, ((0, 16),))
    w_down = gaussian(key_list[19], (EXPERTS, FFE, D), (max(FFE // 64, 1)) ** -0.5, 2.0, ((0, 16),))
    route_ids = draw_route_ids(jax.random.fold_in(jax.random.fold_in(key_list[21], part), 71), part)
    return dict(hidden=hidden, state=state, norm_gain=norm_gain, w_in=w_in, lam_re=lam_re, lam_im=lam_im, log_step=log_step, in_re=in_re, in_im=in_im, out_re=out_re, out_im=out_im, skip=skip, w_glu=w_glu, w_out=w_out, ffn_gain=ffn_gain, w_group=w_group, w_route=w_route, w_gate=w_gate, w_up=w_up, w_down=w_down, route_ids=route_ids)


def normalize(rows, gain):
    wide = rows.astype(jnp.float32)
    return wide * lax.rsqrt(lax.optimization_barrier(jnp.mean(wide * wide, axis=-1, keepdims=True)) + 1e-06) * gain

def discretize(lam_re, lam_im, log_step, in_re, in_im):
    step = jnp.exp(log_step)[:, None]
    magnitude = jnp.exp(lam_re * step)
    bar_re = magnitude * jnp.cos(lam_im * step)
    bar_im = magnitude * jnp.sin(lam_im * step)
    denom = lam_re * lam_re + lam_im * lam_im
    lessened = bar_re - 1.0
    coef_re = (lessened * lam_re + bar_im * lam_im) / denom
    coef_im = (bar_im * lam_re - lessened * lam_im) / denom
    drive_re = coef_re[:, :, None] * in_re - coef_im[:, :, None] * in_im
    drive_im = coef_re[:, :, None] * in_im + coef_im[:, :, None] * in_re
    return (bar_re, bar_im, drive_re, drive_im)

def mixer_step(inputs, state, lam_re, lam_im, log_step, in_re, in_im, out_re, out_im, skip, w_glu):
    rows = inputs.shape[0]
    groups, entries = lam_re.shape
    width = in_re.shape[2]
    highest = lax.Precision.HIGHEST
    bar_re, bar_im, drive_re, drive_im = discretize(lam_re, lam_im, log_step, in_re, in_im)
    wide = inputs.astype(jnp.float32)
    grouped = wide.reshape(rows, groups, width)
    push_re = jnp.einsum('bgc,gnc->bgn', grouped, drive_re, precision=highest)
    push_im = jnp.einsum('bgc,gnc->bgn', grouped, drive_im, precision=highest)
    old_re = state[0].reshape(rows, groups, entries)
    old_im = state[1].reshape(rows, groups, entries)
    new_re = bar_re * old_re - bar_im * old_im + push_re
    new_im = bar_re * old_im + bar_im * old_re + push_im
    read = jnp.einsum('bgn,gcn->bgc', new_re, out_re, precision=highest) - jnp.einsum('bgn,gcn->bgc', new_im, out_im, precision=highest)
    mixed = read.reshape(rows, groups * width) + skip * wide
    active = jax.nn.gelu(mixed)
    gating = jnp.dot(active.astype(jnp.bfloat16), w_glu, preferred_element_type=jnp.float32)
    result = (active * jax.nn.sigmoid(gating)).astype(jnp.bfloat16)
    new_state = jnp.stack([new_re.reshape(rows, -1), new_im.reshape(rows, -1)])
    return (result, new_state)

def route_gates(normed, w_group, w_route, route_ids, per_group):
    group_logit = jnp.dot(normed, w_group, preferred_element_type=jnp.float32)
    route_logit = jnp.dot(normed, w_route, preferred_element_type=jnp.float32)
    chosen = route_ids[:, 0] // per_group
    pick_group = (chosen[:, None] == jnp.arange(group_logit.shape[1], dtype=jnp.int32)[None, :]).astype(jnp.float32)
    own = lax.optimization_barrier(jnp.sum(group_logit * pick_group, axis=1, keepdims=True))
    group_weight = 1.0 / lax.optimization_barrier(jnp.sum(jnp.exp(group_logit - own), axis=1))
    pick = (route_ids[:, :, None] == jnp.arange(route_logit.shape[1], dtype=jnp.int32)[None, None, :]).astype(jnp.float32)
    chosen_logit = lax.optimization_barrier(jnp.sum(pick * route_logit[:, None, :], axis=2))
    first = jax.nn.sigmoid(chosen_logit[:, 0] - chosen_logit[:, 1])
    pair = jnp.stack([first, 1.0 - first], axis=1)
    return group_weight[:, None] * pair

def reference(hidden, state, norm_gain, w_in, lam_re, lam_im, log_step, in_re, in_im, out_re, out_im, skip, w_glu, w_out, ffn_gain, w_group, w_route, w_gate, w_up, w_down, route_ids):
    normed = normalize(hidden, norm_gain).astype(jnp.bfloat16)
    inputs = jnp.dot(normed, w_in, preferred_element_type=jnp.float32).astype(jnp.bfloat16)
    glu, new_state = mixer_step(inputs, state, lam_re, lam_im, log_step, in_re, in_im, out_re, out_im, skip, w_glu)
    resid = (hidden.astype(jnp.float32) + jnp.dot(glu, w_out, preferred_element_type=jnp.float32)).astype(jnp.bfloat16)
    normed2 = normalize(resid, ffn_gain).astype(jnp.bfloat16)
    gates = route_gates(normed2, w_group, w_route, route_ids, EPG)
    limit = N_EP * CAP

    def visit(total, expert):
        hit = route_ids == expert
        weight = lax.optimization_barrier(jnp.sum(jnp.where(hit, gates, 0.0), axis=1))
        used = jnp.any(hit, axis=1)
        count = jnp.sum(used.astype(jnp.int32))
        index = jnp.nonzero(used, size=limit, fill_value=0)[0].astype(jnp.int32)
        valid = (jnp.arange(limit, dtype=jnp.int32) < count).astype(jnp.float32)
        rows = normed2[index]
        gate = jnp.dot(rows, w_gate[expert], preferred_element_type=jnp.float32)
        upper = jnp.dot(rows, w_up[expert], preferred_element_type=jnp.float32)
        inner = (jax.nn.silu(gate) * upper).astype(jnp.bfloat16)
        result = jnp.dot(inner, w_down[expert], preferred_element_type=jnp.float32).astype(jnp.bfloat16)
        scale = weight[index] * valid
        total = total.at[index].add(scale[:, None] * result.astype(jnp.float32))
        return (total, None)
    start = jnp.zeros((hidden.shape[0], hidden.shape[1]), jnp.float32)
    total, unused = lax.scan(visit, start, jnp.arange(EXPERTS, dtype=jnp.int32))
    hidden_out = (resid.astype(jnp.float32) + total).astype(jnp.bfloat16)
    return (hidden_out, new_state)
```

```python
import functools

import jax
import jax.numpy as jnp
from jax import lax
from jax.experimental import pallas as pl
from jax.experimental.pallas import tpu as pltpu
from jax.sharding import PartitionSpec as P

EXP_GROUPS = 4
TOPK = 2
MESH = pl.DeviceIdType.MESH
VMEM = pl.BlockSpec(memory_space=pltpu.VMEM)
ANY = pl.BlockSpec(memory_space=pl.ANY)
F32 = jnp.float32
BF16 = jnp.bfloat16
NT = (((1,), (1,)), ((), ()))
TN = (((0,), (0,)), ((), ()))
LIMIT = 60 * 1024 * 1024


def remote(src, dst, send_sem, recv_sem, device):
    return pltpu.make_async_remote_copy(
        src_ref=src, dst_ref=dst, send_sem=send_sem, recv_sem=recv_sem, device_id=device, device_id_type=MESH
    )


def greet(peers):
    barrier = pltpu.get_barrier_semaphore()
    for peer in peers:
        pl.semaphore_signal(barrier, inc=1, device_id=peer, device_id_type=MESH)
    pl.semaphore_wait(barrier, len(peers))


def gather_kernel(
    chips, hidden_ref, gain_ref, w_ref, out_ref, held, normed, cw_s, cw_r, cc_s, cc_r, x_s, x_r,
    dcw_s, dcw_r, dcc_s, dcc_r, dx_s, dx_r, own_s, own_r, local_sem,
):
    grp = lax.axis_index("grp")
    me = lax.axis_index("ep")
    chip, core = me // 2, me % 2
    half = chips // 2
    odd = chip % 2
    pos = (chip // 2) * (1 - odd) + (chips - 1 - chip // 2) * odd

    def chip_at(place):
        place = (place + 2 * chips) % chips
        upper = place // half
        return 2 * place * (1 - upper) + (2 * (chips - 1 - place) + 1) * upper

    right = (grp, chip_at(pos + 1) * 2 + core)
    left = (grp, chip_at(pos - 1) * 2 + core)
    mate = (grp, me + 1 - 2 * core)
    side = grp % 2
    across = (grp + 1 - 2 * side, me)
    greet([right, left, mate, across])
    rows, depth = w_ref.shape
    third = depth // 3 // 128 * 128
    cw_cols = pl.ds(third, depth - 2 * third)
    cc_cols = pl.ds(pl.multiple_of(side * (depth - third), 128), third)
    x_cols = pl.ds(pl.multiple_of((1 - side) * (depth - third), 128), third)
    subs = 2
    part = rows // subs

    def piece(origin, sub, cols, own=False, who=core):
        span = pl.ds(sub * part, part)
        return w_ref.at[span, cols] if own else held.at[origin, who, span, cols]

    sends = []

    def start(copy):
        copy.start()
        sends.append(copy)

    def cw(step, sub):
        origin = chip_at(pos - step)
        return remote(piece(origin, sub, cw_cols, step == 0), piece(origin, sub, cw_cols), cw_s.at[step, sub], cw_r.at[step, sub], right)

    def cc(step, sub):
        origin = chip_at(pos + step)
        return remote(piece(origin, sub, cc_cols, step == 0), piece(origin, sub, cc_cols), cc_s.at[step, sub], cc_r.at[step, sub], left)

    def cw_in(step, sub):
        spot = piece(chip_at(pos - step - 1), sub, cw_cols)
        return remote(spot, spot, cw_s.at[step, sub], cw_r.at[step, sub], right)

    def cc_in(step, sub):
        spot = piece(chip_at(pos + step + 1), sub, cc_cols)
        return remote(spot, spot, cc_s.at[step, sub], cc_r.at[step, sub], left)

    for sub in range(subs):
        start(cw(0, sub))
        start(cc(0, sub))
    own = remote(w_ref, held.at[chip, core], own_s, own_r, mate)
    start(own)
    local = pltpu.make_async_copy(w_ref, held.at[chip, core], local_sem)
    local.start()

    wide = hidden_ref[...].astype(F32)
    mean = jnp.mean(wide * wide, axis=-1, keepdims=True)
    normed[...] = (wide * lax.rsqrt(mean + 1e-06) * gain_ref[...]).astype(BF16)

    def take_x(step):
        origin = chip_at(pos + step)
        spot = held.at[origin, core, :, x_cols]
        remote(spot, spot, x_s.at[step], x_r.at[step], across).wait_recv()
        start(remote(spot, spot, dx_s.at[step], dx_r.at[step], mate))

    for step in range(1, chips):
        for sub in range(subs):
            cw_in(step - 1, sub).wait_recv()
            if step < chips - 1:
                start(cw(step, sub))
            spot = piece(chip_at(pos - step), sub, cw_cols)
            start(remote(spot, spot, dcw_s.at[step, sub], dcw_r.at[step, sub], mate))
            cc_in(step - 1, sub).wait_recv()
            if step < chips - 1:
                start(cc(step, sub))
            spot = piece(chip_at(pos + step), sub, cc_cols)
            start(remote(spot, spot, dcc_s.at[step, sub], dcc_r.at[step, sub], mate))
        spot = held.at[chip_at(pos + step), core, :, cc_cols]
        start(remote(spot, spot, x_s.at[step], x_r.at[step], across))
        if step >= 2:
            take_x(step - 1)
    take_x(chips - 1)
    other = 1 - core
    for step in range(1, chips):
        for sub in range(subs):
            spot = piece(chip_at(pos - step), sub, cw_cols, False, other)
            remote(spot, spot, dcw_s.at[step, sub], dcw_r.at[step, sub], mate).wait_recv()
            spot = piece(chip_at(pos + step), sub, cc_cols, False, other)
            remote(spot, spot, dcc_s.at[step, sub], dcc_r.at[step, sub], mate).wait_recv()
        spot = held.at[chip_at(pos + step), other, :, x_cols]
        remote(spot, spot, dx_s.at[step], dx_r.at[step], mate).wait_recv()
    spot = held.at[chip, other]
    remote(spot, spot, own_s, own_r, mate).wait_recv()
    local.wait()
    for pair in range(chips // 2):
        block = held[2 * pair : 2 * pair + 2].reshape(4 * rows, depth)
        product = lax.dot_general(normed[...], block, NT, preferred_element_type=F32)
        out_ref[:, 4 * rows * pair : 4 * rows * (pair + 1)] = product.astype(BF16)
    for copy in sends:
        copy.wait_send()


def mixer_kernel(
    per_group, state_ref, inputs_ref, coef_ref, in_re_ref, in_im_ref, out_re_ref, out_im_ref, skip_ref,
    hidden_ref, gain_ref, w_glu_any, w_out_any, w_logit_ref, ids_ref,
    new_ref, resid_ref, rows_ref, place_ref, active, glu_w, out_w, sems,
):
    step = pl.program_id(0)
    steps = pl.num_programs(0)
    width = inputs_ref.shape[1]
    span = state_ref.shape[2]
    entries = out_re_ref.shape[1]
    channels = in_re_ref.shape[1]
    glu_copy = pltpu.make_async_copy(w_glu_any, glu_w, sems.at[0])
    out_copy = pltpu.make_async_copy(w_out_any, out_w, sems.at[1])

    @pl.when(step == 0)
    def _():
        glu_copy.start()
        out_copy.start()

    def iota(shape, axis):
        return lax.broadcasted_iota(jnp.int32, shape, axis)

    spread_in = (iota((channels, width), 1) % channels == iota((channels, width), 0)).astype(BF16)
    mask_in = iota((span, width), 0) // entries == iota((span, width), 1) // channels
    spread_out = (iota((entries, span), 1) % entries == iota((entries, span), 0)).astype(BF16)
    mask_out = iota((width, span), 0) // channels == iota((width, span), 1) // entries

    def block_in(ref):
        tiled = jnp.dot(ref[...].astype(BF16), spread_in, preferred_element_type=F32)
        return jnp.where(mask_in, tiled, 0.0).astype(BF16)

    def block_out(ref):
        tiled = jnp.dot(ref[...].astype(BF16), spread_out, preferred_element_type=F32)
        return jnp.where(mask_out, tiled, 0.0).astype(BF16)

    inputs = inputs_ref[...]
    drive_re = lax.dot_general(inputs, block_in(in_re_ref), NT, preferred_element_type=F32)
    drive_im = lax.dot_general(inputs, block_in(in_im_ref), NT, preferred_element_type=F32)
    bar_re, bar_im = coef_ref[0:1, :], coef_ref[1:2, :]
    coef_re, coef_im = coef_ref[2:3, :], coef_ref[3:4, :]
    old_re, old_im = state_ref[0], state_ref[1]
    new_re = bar_re * old_re - bar_im * old_im + (coef_re * drive_re - coef_im * drive_im)
    new_im = bar_re * old_im + bar_im * old_re + (coef_re * drive_im + coef_im * drive_re)
    new_ref[0] = new_re
    new_ref[1] = new_im
    read = lax.dot_general(new_re.astype(BF16), block_out(out_re_ref), NT, preferred_element_type=F32)
    read = read - lax.dot_general(new_im.astype(BF16), block_out(out_im_ref), NT, preferred_element_type=F32)
    mixed = read + skip_ref[...] * inputs.astype(F32)
    active[:, pl.ds(pl.multiple_of(step * width, 128), width)] = jax.nn.gelu(mixed)

    @pl.when(step == steps - 1)
    def _():
        glu_copy.wait()
        out_copy.wait()
        act = active[...]
        gating = jnp.dot(act.astype(BF16), glu_w[...], preferred_element_type=F32)
        glu = (act * jax.nn.sigmoid(gating)).astype(BF16)
        resid = (hidden_ref[...].astype(F32) + jnp.dot(glu, out_w[...], preferred_element_type=F32)).astype(BF16)
        resid_ref[...] = resid
        wide = resid.astype(F32)
        mean = jnp.mean(wide * wide, axis=-1, keepdims=True)
        normed = (wide * lax.rsqrt(mean + 1e-06) * gain_ref[...]).astype(BF16)
        depth = normed.shape[1]
        rows_ref[:, :depth] = normed
        logits = jnp.dot(normed, w_logit_ref[...], preferred_element_type=F32)
        count = logits.shape[0]
        lane = iota((count, 128), 1)
        first, second = ids_ref[:, 0:1], ids_ref[:, 1:2]
        group = first // per_group
        own = jnp.sum(jnp.where(lane == group, logits, 0.0), axis=1, keepdims=True)
        scale = 1.0 / jnp.sum(jnp.where(lane < EXP_GROUPS, jnp.exp(jnp.where(lane < EXP_GROUPS, logits - own, 0.0)), 0.0), axis=1, keepdims=True)
        r0 = jnp.sum(jnp.where(lane == first + EXP_GROUPS, logits, 0.0), axis=1, keepdims=True)
        r1 = jnp.sum(jnp.where(lane == second + EXP_GROUPS, logits, 0.0), axis=1, keepdims=True)
        share = jax.nn.sigmoid(r0 - r1)
        member = lane % per_group
        gate = jnp.where(member == first % per_group, scale * share, 0.0)
        gate = gate + jnp.where(member == second % per_group, scale * (1.0 - share), 0.0)
        high = gate.astype(BF16).astype(F32)
        packed = jnp.where(lane < per_group, high, jnp.where(lane < 2 * per_group, gate - high, 0.0))
        rows_ref[:, depth:] = packed.astype(BF16)
        hits = (lane == group).astype(BF16)
        earlier = (iota((count, count), 1) < iota((count, count), 0)).astype(BF16)
        before = jnp.dot(earlier, hits, preferred_element_type=F32)
        rank = jnp.sum(jnp.where(lane == group, before, 0.0), axis=1, keepdims=True).astype(jnp.int32)
        slots = place_ref.shape[1]
        slot = group * (slots // EXP_GROUPS) + rank
        place_ref[...] = (iota((count, slots), 1) == slot).astype(BF16)


def expert_kernel(
    groups, per_group, rows_ref, place_ref, resid_ref, gate_any, up_any, down_any, out_ref,
    outgoing, tokens, parts, parts_in, sums, sums_in, final, returned, w_gate, w_up, w_down,
    zs, zr, ys, yr, cs, cr, ps, pr, qs, qr, bs, br, w_sems,
):
    grp = lax.axis_index("grp")
    me = lax.axis_index("ep")
    pairs = per_group // 2
    g, p = me // per_group, me % per_group
    q, c = p // 2, p % 2
    depth = resid_ref.shape[1]
    cap = outgoing.shape[1]
    wide = outgoing.shape[2]

    def at(group, pair):
        return (grp, group * per_group + pair * 2 + c)

    mate = (grp, me + 1 - 2 * c)
    others = [(g + i) % groups for i in range(1, groups)]
    mates_q = [(q + j) % pairs for j in range(1, pairs)]
    loads = [
        pltpu.make_async_copy(gate_any.at[0], w_gate, w_sems.at[0]),
        pltpu.make_async_copy(up_any.at[0], w_up, w_sems.at[1]),
        pltpu.make_async_copy(down_any.at[0], w_down, w_sems.at[2]),
    ]
    for load in loads:
        load.start()
    sent = lax.dot_general(place_ref[...], rows_ref[...], TN, preferred_element_type=F32).astype(BF16)
    outgoing[...] = sent.reshape(groups, cap, wide)
    tokens[g, c, q] = outgoing[g]
    greet([at(o, q) for o in others] + [at(g, o) for o in mates_q] + [mate])
    sends = []

    def start(copy):
        copy.start()
        sends.append(copy)

    for target in others:
        start(remote(outgoing.at[target], tokens.at[g, c, q], zs.at[target], zr.at[g], at(target, q)))

    def source(i):
        return (g + groups - i) % groups

    def to_mate(s, pair):
        spot = tokens.at[s, c, pair]
        start(remote(spot, spot, cs.at[s, pair], cr.at[s, pair], mate))

    def stage_a(i):
        s = source(i)
        spot = tokens.at[s, c, q]
        if i > 0:
            remote(spot, spot, zs.at[s], zr.at[s], mate).wait_recv()
        for o in mates_q:
            start(remote(spot, spot, ys.at[s, o], yr.at[s, q], at(g, o)))
        to_mate(s, q)

    def stage_b(i):
        s = source(i)
        for o in mates_q:
            spot = tokens.at[s, c, o]
            remote(spot, spot, ys.at[s, o], yr.at[s, o], mate).wait_recv()
            to_mate(s, o)

    def stage_c(i):
        s = source(i)
        for o in range(pairs):
            spot = tokens.at[s, 1 - c, o]
            remote(spot, spot, cs.at[s, o], cr.at[s, o], mate).wait_recv()
        if i == 0:
            for load in loads:
                load.wait()
        total = per_group * cap
        x = tokens[s].reshape(total, wide)
        rows = x[:, :depth]
        gate = jnp.dot(rows, w_gate[...], preferred_element_type=F32)
        upper = jnp.dot(rows, w_up[...], preferred_element_type=F32)
        inner = (jax.nn.silu(gate) * upper).astype(BF16)
        result = jnp.dot(inner, w_down[...], preferred_element_type=F32).astype(BF16)
        lane = lax.broadcasted_iota(jnp.int32, (total, wide - depth), 1)
        mine = (lane == p) | (lane == p + per_group)
        weight = jnp.sum(jnp.where(mine, x[:, depth:].astype(F32), 0.0), axis=1, keepdims=True)
        parts[s] = (result.astype(F32) * weight).astype(BF16).reshape(2, pairs, cap, depth)
        start(remote(parts.at[s, 1 - c], parts_in.at[s], ps.at[s], pr.at[s], mate))

    def stage_d(i):
        s = source(i)
        spot = parts_in.at[s]
        remote(spot, spot, ps.at[s], pr.at[s], mate).wait_recv()
        sums[s] = (parts[s, c].astype(F32) + parts_in[s].astype(F32)).astype(BF16)
        for o in mates_q:
            start(remote(sums.at[s, o], sums_in.at[s, q], qs.at[s, o], qr.at[s, q], at(g, o)))

    def stage_e(i):
        s = source(i)
        total = sums[s, q].astype(F32)
        for o in mates_q:
            spot = sums_in.at[s, o]
            remote(spot, spot, qs.at[s, o], qr.at[s, o], mate).wait_recv()
            total = total + sums_in[s, o].astype(F32)
        if i == 0:
            returned[g] = total.astype(BF16)
        else:
            final[s] = total.astype(BF16)
            start(remote(final.at[s], returned.at[g], bs.at[s], br.at[g], at(s, q)))

    stage_a(0)
    for t in range(groups):
        stage_b(t)
        if t + 1 < groups:
            stage_a(t + 1)
        stage_c(t)
        stage_d(t)
        if t > 0:
            stage_e(t - 1)
    stage_e(groups - 1)
    for o in others:
        spot = returned.at[o]
        remote(spot, spot, bs.at[o], br.at[o], mate).wait_recv()
    back = returned[...].reshape(groups * cap, depth)
    moe = jnp.dot(place_ref[...], back, preferred_element_type=F32)
    out_ref[...] = (resid_ref[...].astype(F32) + moe).astype(BF16)
    for copy in sends:
        copy.wait_send()


def on_device(
    hidden, state, norm_gain, w_in, lam_re, lam_im, log_step, in_re, in_im, out_re, out_im, skip, w_glu, w_out,
    ffn_gain, w_group, w_route, w_gate, w_up, w_down, route_ids,
):
    rows, depth = hidden.shape
    devices = lax.axis_size("ep")
    chips = devices // 2
    shard = w_in.shape[1]
    dma = pltpu.SemaphoreType.DMA
    inputs = pl.pallas_call(
        functools.partial(gather_kernel, chips),
        out_shape=jax.ShapeDtypeStruct((rows, shard * devices), BF16),
        in_specs=[VMEM] * 3,
        out_specs=VMEM,
        scratch_shapes=[pltpu.VMEM((chips, 2, shard, depth), BF16), pltpu.VMEM((rows, depth), BF16)]
        + [dma((chips, 2))] * 4 + [dma((chips,))] * 2 + [dma((chips, 2))] * 4 + [dma((chips,))] * 2
        + [dma, dma, dma],
        compiler_params=pltpu.CompilerParams(collective_id=0, has_side_effects=True, vmem_limit_bytes=LIMIT),
        name="gather_in",
    )(hidden, norm_gain[None, :], w_in.T)

    groups, entries = lam_re.shape
    width = in_re.shape[2]
    flat = groups * entries
    lr, li = lam_re.reshape(1, flat), lam_im.reshape(1, flat)
    step = jnp.exp(jnp.broadcast_to(log_step[:, None], (groups, entries)).reshape(1, flat))
    magnitude = jnp.exp(lr * step)
    bar_re = magnitude * jnp.cos(li * step)
    bar_im = magnitude * jnp.sin(li * step)
    denom = lr * lr + li * li
    lessened = bar_re - 1.0
    coef = jnp.concatenate(
        [bar_re, bar_im, (lessened * lr + bar_im * li) / denom, (bar_im * lr - lessened * li) / denom], axis=0
    )
    experts = w_route.shape[1]
    per_group = experts // EXP_GROUPS
    w_logit = jnp.concatenate(
        [w_group, w_route, jnp.zeros((depth, 128 - EXP_GROUPS - experts), BF16)], axis=1
    )
    cap = 2 * rows // EXP_GROUPS
    block = 128 // width
    span = block * entries
    channels = groups * width
    const = lambda *shape: pl.BlockSpec(shape, lambda i: (0,) * len(shape))
    new_state, resid, packed, place = pl.pallas_call(
        functools.partial(mixer_kernel, per_group),
        grid=(groups // block,),
        out_shape=[
            jax.ShapeDtypeStruct(state.shape, F32),
            jax.ShapeDtypeStruct((rows, depth), BF16),
            jax.ShapeDtypeStruct((rows, depth + 128), BF16),
            jax.ShapeDtypeStruct((rows, EXP_GROUPS * cap), BF16),
        ],
        in_specs=[
            pl.BlockSpec((2, rows, span), lambda i: (0, 0, i)),
            pl.BlockSpec((rows, 128), lambda i: (0, i)),
            pl.BlockSpec((4, span), lambda i: (0, i)),
            pl.BlockSpec((span, width), lambda i: (i, 0)),
            pl.BlockSpec((span, width), lambda i: (i, 0)),
            pl.BlockSpec((128, entries), lambda i: (i, 0)),
            pl.BlockSpec((128, entries), lambda i: (i, 0)),
            pl.BlockSpec((1, 128), lambda i: (0, i)),
            const(rows, depth),
            const(1, depth),
            ANY,
            ANY,
            const(depth, 128),
            const(rows, TOPK),
        ],
        out_specs=[
            pl.BlockSpec((2, rows, span), lambda i: (0, 0, i)),
            const(rows, depth),
            const(rows, depth + 128),
            const(rows, EXP_GROUPS * cap),
        ],
        scratch_shapes=[
            pltpu.VMEM((rows, channels), F32),
            pltpu.VMEM(w_glu.shape, BF16),
            pltpu.VMEM(w_out.shape, BF16),
            dma((2,)),
        ],
        compiler_params=pltpu.CompilerParams(dimension_semantics=("arbitrary",), vmem_limit_bytes=LIMIT),
        name="mixer",
    )(
        state, inputs, coef, in_re.reshape(flat, width), in_im.reshape(flat, width),
        out_re.reshape(channels, entries), out_im.reshape(channels, entries), skip[None, :],
        hidden, ffn_gain[None, :], w_glu, w_out, w_logit, route_ids,
    )

    pairs = per_group // 2
    G = EXP_GROUPS
    hidden_out = pl.pallas_call(
        functools.partial(expert_kernel, G, per_group),
        out_shape=jax.ShapeDtypeStruct((rows, depth), BF16),
        in_specs=[VMEM] * 3 + [ANY] * 3,
        out_specs=VMEM,
        scratch_shapes=[
            pltpu.VMEM((G, cap, depth + 128), BF16),
            pltpu.VMEM((G, 2, pairs, cap, depth + 128), BF16),
            pltpu.VMEM((G, 2, pairs, cap, depth), BF16),
            pltpu.VMEM((G, pairs, cap, depth), BF16),
            pltpu.VMEM((G, pairs, cap, depth), BF16),
            pltpu.VMEM((G, pairs, cap, depth), BF16),
            pltpu.VMEM((G, cap, depth), BF16),
            pltpu.VMEM((G, cap, depth), BF16),
            pltpu.VMEM(w_gate.shape[1:], BF16),
            pltpu.VMEM(w_up.shape[1:], BF16),
            pltpu.VMEM(w_down.shape[1:], BF16),
            dma((G,)), dma((G,)), dma((G, pairs)), dma((G, pairs)), dma((G, pairs)), dma((G, pairs)),
            dma((G,)), dma((G,)), dma((G, pairs)), dma((G, pairs)), dma((G,)), dma((G,)), dma((3,)),
        ],
        compiler_params=pltpu.CompilerParams(collective_id=1, has_side_effects=True, vmem_limit_bytes=LIMIT),
        name="experts",
    )(packed, place, resid, w_gate, w_up, w_down)
    return (hidden_out, new_state)


def solution(mesh):
    return jax.shard_map(
        on_device,
        mesh=mesh,
        in_specs=(
            P(("grp", "ep"), None),
            P(None, ("grp", "ep"), None),
            P(),
            P(None, "ep"),
            P(),
            P(),
            P(),
            P(),
            P(),
            P(),
            P(),
            P(),
            P(),
            P(),
            P(),
            P(),
            P(),
            P("ep", None, None),
            P("ep", None, None),
            P("ep", None, None),
            P(("grp", "ep"), None),
        ),
        out_specs=(P(("grp", "ep"), None), P(None, ("grp", "ep"), None)),
        check_vma=False,
    )
```

```python
import functools

import jax
import jax.numpy as jnp
from jax import lax
from jax.experimental import pallas as pl
from jax.experimental.pallas import tpu as pltpu
from jax.sharding import PartitionSpec as P

EXP_GROUPS = 4
TOPK = 2
MESH = pl.DeviceIdType.MESH
VMEM = pl.BlockSpec(memory_space=pltpu.VMEM)
ANY = pl.BlockSpec(memory_space=pl.ANY)
F32 = jnp.float32
BF16 = jnp.bfloat16
NT = (((1,), (1,)), ((), ()))
TN = (((0,), (0,)), ((), ()))
LIMIT = 60 * 1024 * 1024


def remote(src, dst, send_sem, recv_sem, device):
    return pltpu.make_async_remote_copy(
        src_ref=src, dst_ref=dst, send_sem=send_sem, recv_sem=recv_sem, device_id=device, device_id_type=MESH
    )


def greet(peers):
    barrier = pltpu.get_barrier_semaphore()
    for peer in peers:
        pl.semaphore_signal(barrier, inc=1, device_id=peer, device_id_type=MESH)
    pl.semaphore_wait(barrier, len(peers))


def gather_kernel(
    chips, hidden_ref, gain_ref, w_ref, out_ref, held, normed, zs, zr, ys, yr, xs, xr, ds, dr, es, er,
    own_s, own_r, local_sem,
):
    grp = lax.axis_index("grp")
    me = lax.axis_index("ep")
    chip, core = me // 2, me % 2
    lines = chips // 2
    line, y = chip // 2, chip % 2

    def at(row, column):
        return (grp, (row * 2 + column) * 2 + core)

    targets = [(line + i) % lines for i in range(1, lines)]
    mate = (grp, me + 1 - 2 * core)
    side = grp % 2
    across = (grp + 1 - 2 * side, me)
    beside = at(line, 1 - y)
    rows, depth = w_ref.shape
    third = depth // 3 // 128 * 128
    my_cols = pl.ds(pl.multiple_of(side * third, 128), depth - third)
    out_cols = pl.ds(pl.multiple_of(side * (depth - third), 128), third)
    in_cols = pl.ds(pl.multiple_of((1 - side) * (depth - third), 128), third)
    subs = 2
    part = rows // subs
    spans = [pl.ds(sub * part, part) for sub in range(subs)]
    sends = []

    def start(copy):
        copy.start()
        sends.append(copy)

    local = pltpu.make_async_copy(w_ref, held.at[chip, core], local_sem)
    local.start()
    greet([at(target, y) for target in targets] + [beside, mate, across])
    for i in range(lines):
        for sub in range(subs):
            src, dst = w_ref.at[spans[sub], my_cols], held.at[chip, core, spans[sub], my_cols]
            if i == 0:
                start(remote(src, dst, ys.at[0, sub], yr.at[0, sub], beside))
            else:
                start(remote(src, dst, zs.at[i, sub], zr.at[i, sub], at(targets[i - 1], y)))
    start(remote(w_ref, held.at[chip, core], own_s, own_r, mate))

    wide = hidden_ref[...].astype(F32)
    mean = jnp.mean(wide * wide, axis=-1, keepdims=True)
    normed[...] = (wide * lax.rsqrt(mean + 1e-06) * gain_ref[...]).astype(BF16)

    def origin(kind, i):
        return (line + lines - i) % lines * 2 + (y if kind == 0 else 1 - y)

    order = []
    for i in range(1, lines + 1):
        for sub in range(subs):
            if i < lines:
                order.append((0, i, sub))
            order.append((1, i - 1, sub))

    def take(kind, i, sub):
        place = origin(kind, i)
        spot = held.at[place, core, spans[sub], my_cols]
        if kind == 0:
            remote(spot, spot, zs.at[i, sub], zr.at[i, sub], mate).wait_recv()
            start(remote(spot, spot, ys.at[i, sub], yr.at[i, sub], beside))
        else:
            remote(spot, spot, ys.at[i, sub], yr.at[i, sub], mate).wait_recv()
        side_spot = held.at[place, core, spans[sub], out_cols]
        start(remote(side_spot, side_spot, xs.at[kind, i, sub], xr.at[kind, i, sub], across))
        start(remote(spot, spot, ds.at[kind, i, sub], dr.at[kind, i, sub], mate))

    def take_x(kind, i, sub):
        spot = held.at[origin(kind, i), core, spans[sub], in_cols]
        remote(spot, spot, xs.at[kind, i, sub], xr.at[kind, i, sub], mate).wait_recv()
        start(remote(spot, spot, es.at[kind, i, sub], er.at[kind, i, sub], mate))

    lag = 2 * subs
    for at_ in range(len(order) + lag):
        if at_ < len(order):
            take(*order[at_])
        if at_ >= lag:
            take_x(*order[at_ - lag])
    for kind, i, sub in order:
        place = origin(kind, i)
        spot = held.at[place, 1 - core, spans[sub], my_cols]
        remote(spot, spot, ds.at[kind, i, sub], dr.at[kind, i, sub], mate).wait_recv()
        spot = held.at[place, 1 - core, spans[sub], in_cols]
        remote(spot, spot, es.at[kind, i, sub], er.at[kind, i, sub], mate).wait_recv()
    spot = held.at[chip, 1 - core]
    remote(spot, spot, own_s, own_r, mate).wait_recv()
    local.wait()
    for pair in range(chips // 2):
        block = held[2 * pair : 2 * pair + 2].reshape(4 * rows, depth)
        product = lax.dot_general(normed[...], block, NT, preferred_element_type=F32)
        out_ref[:, 4 * rows * pair : 4 * rows * (pair + 1)] = product.astype(BF16)
    for copy in sends:
        copy.wait_send()


def mixer_kernel(
    per_group, state_ref, inputs_ref, coef_ref, in_re_ref, in_im_ref, out_re_ref, out_im_ref, skip_ref,
    hidden_ref, gain_ref, w_glu_any, w_out_any, w_group_ref, w_route_ref, ids_ref,
    new_ref, resid_ref, rows_ref, place_ref, active, glu_w, out_w, sems,
):
    step = pl.program_id(0)
    steps = pl.num_programs(0)
    width = inputs_ref.shape[1]
    span = state_ref.shape[2]
    entries = out_re_ref.shape[1]
    channels = width // (span // entries)
    glu_copy = pltpu.make_async_copy(w_glu_any, glu_w, sems.at[0])
    out_copy = pltpu.make_async_copy(w_out_any, out_w, sems.at[1])

    @pl.when(step == 0)
    def _():
        glu_copy.start()
        out_copy.start()

    def iota(shape, axis):
        return lax.broadcasted_iota(jnp.int32, shape, axis)

    spread_out = (iota((entries, span), 1) % entries == iota((entries, span), 0)).astype(BF16)
    mask_out = iota((width, span), 0) // channels == iota((width, span), 1) // entries

    def block(ref):
        tiled = jnp.dot(ref[...].astype(BF16), spread_out, preferred_element_type=F32)
        return jnp.where(mask_out, tiled, 0.0).astype(BF16)

    inputs = inputs_ref[...]
    drive_re = jnp.dot(inputs, block(in_re_ref), preferred_element_type=F32)
    drive_im = jnp.dot(inputs, block(in_im_ref), preferred_element_type=F32)
    bar_re, bar_im = coef_ref[0:1, :], coef_ref[1:2, :]
    coef_re, coef_im = coef_ref[2:3, :], coef_ref[3:4, :]
    old_re, old_im = state_ref[0], state_ref[1]
    new_re = bar_re * old_re - bar_im * old_im + (coef_re * drive_re - coef_im * drive_im)
    new_im = bar_re * old_im + bar_im * old_re + (coef_re * drive_im + coef_im * drive_re)
    new_ref[0] = new_re
    new_ref[1] = new_im
    read = lax.dot_general(new_re.astype(BF16), block(out_re_ref), NT, preferred_element_type=F32)
    read = read - lax.dot_general(new_im.astype(BF16), block(out_im_ref), NT, preferred_element_type=F32)
    mixed = read + skip_ref[...] * inputs.astype(F32)
    active[:, pl.ds(pl.multiple_of(step * width, 128), width)] = jax.nn.gelu(mixed)

    @pl.when(step == steps - 1)
    def _():
        glu_copy.wait()
        out_copy.wait()
        act = active[...]
        gating = jnp.dot(act.astype(BF16), glu_w[...], preferred_element_type=F32)
        glu = (act * jax.nn.sigmoid(gating)).astype(BF16)
        resid = (hidden_ref[...].astype(F32) + jnp.dot(glu, out_w[...], preferred_element_type=F32)).astype(BF16)
        resid_ref[...] = resid
        wide = resid.astype(F32)
        mean = jnp.mean(wide * wide, axis=-1, keepdims=True)
        normed = (wide * lax.rsqrt(mean + 1e-06) * gain_ref[...]).astype(BF16)
        depth = normed.shape[1]
        rows_ref[:, :depth] = normed
        level = lax.dot_general(normed, w_group_ref[...], NT, preferred_element_type=F32)
        logits = lax.dot_general(normed, w_route_ref[...], NT, preferred_element_type=F32)
        count = normed.shape[0]
        lane = iota((count, 128), 1)
        same = (iota((count, count), 0) == iota((count, count), 1)).astype(BF16)
        ids = lax.dot_general(same, ids_ref[...].astype(F32).astype(BF16), NT, preferred_element_type=F32).astype(jnp.int32)
        first, second = ids[:, 0:1], ids[:, 1:2]
        group = first // per_group
        own = jnp.sum(jnp.where(iota(level.shape, 1) == group, level, 0.0), axis=1, keepdims=True)
        scale = 1.0 / jnp.sum(jnp.exp(level - own), axis=1, keepdims=True)
        r0 = jnp.sum(jnp.where(iota(logits.shape, 1) == first, logits, 0.0), axis=1, keepdims=True)
        r1 = jnp.sum(jnp.where(iota(logits.shape, 1) == second, logits, 0.0), axis=1, keepdims=True)
        share = jax.nn.sigmoid(r0 - r1)
        member = lane % per_group
        gate = jnp.where(member == first % per_group, scale * share, 0.0)
        gate = gate + jnp.where(member == second % per_group, scale * (1.0 - share), 0.0)
        high = gate.astype(BF16).astype(F32)
        packed = jnp.where(lane < per_group, high, jnp.where(lane < 2 * per_group, gate - high, 0.0))
        rows_ref[:, depth:] = packed.astype(BF16)
        hits = (lane == group).astype(BF16)
        earlier = (iota((count, count), 1) < iota((count, count), 0)).astype(BF16)
        before = jnp.dot(earlier, hits, preferred_element_type=F32)
        rank = jnp.sum(jnp.where(lane == group, before, 0.0), axis=1, keepdims=True).astype(jnp.int32)
        slots = place_ref.shape[1]
        slot = group * (slots // EXP_GROUPS) + rank
        place_ref[...] = (iota((count, slots), 1) == slot).astype(BF16)


def expert_kernel(
    groups, per_group, rows_ref, place_ref, resid_ref, gate_any, up_any, down_any, out_ref,
    outgoing, tokens, parts, parts_in, sums, sums_in, final, returned, w_gate, w_up, w_down,
    zs, zr, ys, yr, cs, cr, ps, pr, qs, qr, bs, br, w_sems,
):
    grp = lax.axis_index("grp")
    me = lax.axis_index("ep")
    pairs = per_group // 2
    g, p = me // per_group, me % per_group
    q, c = p // 2, p % 2
    depth = resid_ref.shape[1]
    cap = outgoing.shape[1]
    wide = outgoing.shape[2]

    def at(group, pair):
        return (grp, group * per_group + pair * 2 + c)

    mate = (grp, me + 1 - 2 * c)
    others = [(g + i) % groups for i in range(1, groups)]
    mates_q = [(q + j) % pairs for j in range(1, pairs)]
    loads = [
        pltpu.make_async_copy(gate_any.at[0], w_gate, w_sems.at[0]),
        pltpu.make_async_copy(up_any.at[0], w_up, w_sems.at[1]),
        pltpu.make_async_copy(down_any.at[0], w_down, w_sems.at[2]),
    ]
    for load in loads:
        load.start()
    sent = lax.dot_general(place_ref[...], rows_ref[...], TN, preferred_element_type=F32).astype(BF16)
    outgoing[...] = sent.reshape(groups, cap, wide)
    tokens[g, c, q] = outgoing[g]
    greet([at(o, q) for o in others] + [at(g, o) for o in mates_q] + [mate])
    sends = []

    def start(copy):
        copy.start()
        sends.append(copy)

    for target in others:
        start(remote(outgoing.at[target], tokens.at[g, c, q], zs.at[target], zr.at[g], at(target, q)))

    def source(i):
        return (g + groups - i) % groups

    def to_mate(s, pair):
        spot = tokens.at[s, c, pair]
        start(remote(spot, spot, cs.at[s, pair], cr.at[s, pair], mate))

    def stage_a(i):
        s = source(i)
        spot = tokens.at[s, c, q]
        if i > 0:
            remote(spot, spot, zs.at[s], zr.at[s], mate).wait_recv()
        for o in mates_q:
            start(remote(spot, spot, ys.at[s, o], yr.at[s, q], at(g, o)))
        to_mate(s, q)

    def stage_b(i):
        s = source(i)
        for o in mates_q:
            spot = tokens.at[s, c, o]
            remote(spot, spot, ys.at[s, o], yr.at[s, o], mate).wait_recv()
            to_mate(s, o)

    def stage_c(i):
        s = source(i)
        for o in range(pairs):
            spot = tokens.at[s, 1 - c, o]
            remote(spot, spot, cs.at[s, o], cr.at[s, o], mate).wait_recv()
        if i == 0:
            for load in loads:
                load.wait()
        total = per_group * cap
        x = tokens[s].reshape(total, wide)
        rows = x[:, :depth]
        gate = jnp.dot(rows, w_gate[...], preferred_element_type=F32)
        upper = jnp.dot(rows, w_up[...], preferred_element_type=F32)
        inner = (jax.nn.silu(gate) * upper).astype(BF16)
        result = jnp.dot(inner, w_down[...], preferred_element_type=F32).astype(BF16)
        lane = lax.broadcasted_iota(jnp.int32, (total, wide - depth), 1)
        mine = (lane == p) | (lane == p + per_group)
        weight = jnp.sum(jnp.where(mine, x[:, depth:].astype(F32), 0.0), axis=1, keepdims=True)
        parts[s] = (result.astype(F32) * weight).astype(BF16).reshape(2, pairs, cap, depth)
        start(remote(parts.at[s, 1 - c], parts_in.at[s], ps.at[s], pr.at[s], mate))

    def stage_d(i):
        s = source(i)
        spot = parts_in.at[s]
        remote(spot, spot, ps.at[s], pr.at[s], mate).wait_recv()
        sums[s] = (parts[s, c].astype(F32) + parts_in[s].astype(F32)).astype(BF16)
        for o in mates_q:
            start(remote(sums.at[s, o], sums_in.at[s, q], qs.at[s, o], qr.at[s, q], at(g, o)))

    def stage_e(i):
        s = source(i)
        total = sums[s, q].astype(F32)
        for o in mates_q:
            spot = sums_in.at[s, o]
            remote(spot, spot, qs.at[s, o], qr.at[s, o], mate).wait_recv()
            total = total + sums_in[s, o].astype(F32)
        if i == 0:
            returned[g] = total.astype(BF16)
        else:
            final[s] = total.astype(BF16)
            start(remote(final.at[s], returned.at[g], bs.at[s], br.at[g], at(s, q)))

    stage_a(0)
    for t in range(groups):
        stage_b(t)
        if t + 1 < groups:
            stage_a(t + 1)
        stage_c(t)
        stage_d(t)
        if t > 0:
            stage_e(t - 1)
    stage_e(groups - 1)
    for o in others:
        spot = returned.at[o]
        remote(spot, spot, bs.at[o], br.at[o], mate).wait_recv()
    back = returned[...].reshape(groups * cap, depth)
    moe = jnp.dot(place_ref[...], back, preferred_element_type=F32)
    out_ref[...] = (resid_ref[...].astype(F32) + moe).astype(BF16)
    for copy in sends:
        copy.wait_send()


def on_device(
    hidden, state, norm_gain, w_in, lam_re, lam_im, log_step, in_re, in_im, out_re, out_im, skip, w_glu, w_out,
    ffn_gain, w_group, w_route, w_gate, w_up, w_down, route_ids,
):
    rows, depth = hidden.shape
    devices = lax.axis_size("ep")
    chips = devices // 2
    shard = w_in.shape[1]
    dma = pltpu.SemaphoreType.DMA
    inputs = pl.pallas_call(
        functools.partial(gather_kernel, chips),
        out_shape=jax.ShapeDtypeStruct((rows, shard * devices), BF16),
        in_specs=[VMEM] * 3,
        out_specs=VMEM,
        scratch_shapes=[pltpu.VMEM((chips, 2, shard, depth), BF16), pltpu.VMEM((rows, depth), BF16)]
        + [dma((chips // 2, 2))] * 4 + [dma((2, chips // 2, 2))] * 6 + [dma, dma, dma],
        compiler_params=pltpu.CompilerParams(collective_id=0, has_side_effects=True, vmem_limit_bytes=LIMIT),
        name="gather_in",
    )(hidden, norm_gain[None, :], w_in.T)

    groups, entries = lam_re.shape
    width = in_re.shape[2]
    flat = groups * entries
    lr, li = lam_re.reshape(1, flat), lam_im.reshape(1, flat)
    step = jnp.exp(jnp.broadcast_to(log_step[:, None], (groups, entries)).reshape(1, flat))
    magnitude = jnp.exp(lr * step)
    bar_re = magnitude * jnp.cos(li * step)
    bar_im = magnitude * jnp.sin(li * step)
    denom = lr * lr + li * li
    lessened = bar_re - 1.0
    coef = jnp.concatenate(
        [bar_re, bar_im, (lessened * lr + bar_im * li) / denom, (bar_im * lr - lessened * li) / denom], axis=0
    )
    experts = w_route.shape[1]
    per_group = experts // EXP_GROUPS
    cap = 2 * rows // EXP_GROUPS
    block = 128 // width
    span = block * entries
    channels = groups * width
    const = lambda *shape: pl.BlockSpec(shape, lambda i: (0,) * len(shape))
    new_state, resid, packed, place = pl.pallas_call(
        functools.partial(mixer_kernel, per_group),
        grid=(groups // block,),
        out_shape=[
            jax.ShapeDtypeStruct(state.shape, F32),
            jax.ShapeDtypeStruct((rows, depth), BF16),
            jax.ShapeDtypeStruct((rows, depth + 128), BF16),
            jax.ShapeDtypeStruct((rows, EXP_GROUPS * cap), BF16),
        ],
        in_specs=[
            pl.BlockSpec((2, rows, span), lambda i: (0, 0, i)),
            pl.BlockSpec((rows, 128), lambda i: (0, i)),
            pl.BlockSpec((4, span), lambda i: (0, i)),
            pl.BlockSpec((128, entries), lambda i: (i, 0)),
            pl.BlockSpec((128, entries), lambda i: (i, 0)),
            pl.BlockSpec((128, entries), lambda i: (i, 0)),
            pl.BlockSpec((128, entries), lambda i: (i, 0)),
            pl.BlockSpec((1, 128), lambda i: (0, i)),
            const(rows, depth),
            const(1, depth),
            ANY,
            ANY,
            const(EXP_GROUPS, depth),
            const(experts, depth),
            const(TOPK, rows),
        ],
        out_specs=[
            pl.BlockSpec((2, rows, span), lambda i: (0, 0, i)),
            const(rows, depth),
            const(rows, depth + 128),
            const(rows, EXP_GROUPS * cap),
        ],
        scratch_shapes=[
            pltpu.VMEM((rows, channels), F32),
            pltpu.VMEM(w_glu.shape, BF16),
            pltpu.VMEM(w_out.shape, BF16),
            dma((2,)),
        ],
        compiler_params=pltpu.CompilerParams(dimension_semantics=("arbitrary",), vmem_limit_bytes=LIMIT),
        name="mixer",
    )(
        state, inputs, coef, in_re.transpose(0, 2, 1).reshape(channels, entries),
        in_im.transpose(0, 2, 1).reshape(channels, entries),
        out_re.reshape(channels, entries), out_im.reshape(channels, entries), skip[None, :],
        hidden, ffn_gain[None, :], w_glu, w_out, w_group.T, w_route.T, route_ids.T,
    )

    pairs = per_group // 2
    G = EXP_GROUPS
    hidden_out = pl.pallas_call(
        functools.partial(expert_kernel, G, per_group),
        out_shape=jax.ShapeDtypeStruct((rows, depth), BF16),
        in_specs=[VMEM] * 3 + [ANY] * 3,
        out_specs=VMEM,
        scratch_shapes=[
            pltpu.VMEM((G, cap, depth + 128), BF16),
            pltpu.VMEM((G, 2, pairs, cap, depth + 128), BF16),
            pltpu.VMEM((G, 2, pairs, cap, depth), BF16),
            pltpu.VMEM((G, pairs, cap, depth), BF16),
            pltpu.VMEM((G, pairs, cap, depth), BF16),
            pltpu.VMEM((G, pairs, cap, depth), BF16),
            pltpu.VMEM((G, cap, depth), BF16),
            pltpu.VMEM((G, cap, depth), BF16),
            pltpu.VMEM(w_gate.shape[1:], BF16),
            pltpu.VMEM(w_up.shape[1:], BF16),
            pltpu.VMEM(w_down.shape[1:], BF16),
            dma((G,)), dma((G,)), dma((G, pairs)), dma((G, pairs)), dma((G, pairs)), dma((G, pairs)),
            dma((G,)), dma((G,)), dma((G, pairs)), dma((G, pairs)), dma((G,)), dma((G,)), dma((3,)),
        ],
        compiler_params=pltpu.CompilerParams(collective_id=1, has_side_effects=True, vmem_limit_bytes=LIMIT),
        name="experts",
    )(packed, place, resid, w_gate, w_up, w_down)
    return (hidden_out, new_state)


def solution(mesh):
    return jax.shard_map(
        on_device,
        mesh=mesh,
        in_specs=(
            P(("grp", "ep"), None),
            P(None, ("grp", "ep"), None),
            P(),
            P(None, "ep"),
            P(),
            P(),
            P(),
            P(),
            P(),
            P(),
            P(),
            P(),
            P(),
            P(),
            P(),
            P(),
            P(),
            P("ep", None, None),
            P("ep", None, None),
            P("ep", None, None),
            P(("grp", "ep"), None),
        ),
        out_specs=(P(("grp", "ep"), None), P(None, ("grp", "ep"), None)),
        check_vma=False,
    )
```
